32 devices in a mesh: ra: 2 (over core), cb: 4 (over z), dp: 4 (over y, x).
Axes of the slice: x: 2, y: 2, z: 4, core: 2. Of those that a mesh axis runs over, the one named last changes fastest.
Arguments:
- residual_in: bfloat16 [1024, 4096], P('dp', 'cb'), may hold values from -220 to 220, as said below
- gain_in: float32 [4096], P('cb'), may hold values from 0.1 to 1.9
- shift_in: float32 [4096], P('cb'), may hold values from -3 to 3
- up_weight: bfloat16 [4096, 16384], P('cb', 'ra'), may hold values from -0.09375 to 0.09375
- down_weight: bfloat16 [16384, 4096], P('ra', 'cb'), may hold values from -0.046875 to 0.046875
- gain_out: float32 [4096], P('cb'), may hold values from 0.1 to 1.9
- shift_out: float32 [4096], P('cb'), may hold values from -3 to 3
Outputs:
- layer_out: bfloat16 [1024, 4096], P('dp', 'cb')
The draws below stay inside these ranges and needn't reach their ends.
Inputs may be any that keep to these rules, and one draw needn't show every extreme that they name: `residual_in`: real-valued activations.
All inputs are finite; a program needn't handle non-finite values.
Results may differ from the reference program's by a relative error of at most 0.0065.
Values may be sent and summed in bfloat16 or wider, within the bound.
A program may use at most 128 MiB of HBM per device.

```python
import jax
import jax.numpy as jnp
from jax import lax

D = 4096
FF = 16384
TOKENS = 1024


def draw_residual_in(key, part):
    first, second, third = jax.random.split(key, 3)
    column = jnp.arange(D, dtype=jnp.float32) / D
    colscale = 0.5 * jnp.exp(jnp.log(6.0) * column) * jnp.exp(jax.random.uniform(second, (D,), jnp.float32, -0.35, 0.35))
    rowscale = jnp.exp(jax.random.uniform(third, (TOKENS, 1), jnp.float32, 0.0, jnp.log(10.0)))
    noise = jnp.clip(jax.random.normal(first, (TOKENS, D), jnp.float32), -5.0, 5.0)
    values = rowscale * noise * colscale
    return values.astype(jnp.bfloat16)


def steps_of(stream_key, dims, shards, low, high):
    level = 1.0
    for axis_at, parts in shards:
        heights = jax.random.uniform(jax.random.fold_in(jax.random.fold_in(stream_key, 6), axis_at), (parts,), jnp.float32, low / len(shards), high / len(shards))
        level = level * jnp.repeat(jnp.exp(heights), dims[axis_at] // parts).reshape((-1,) + (1,) * (len(dims) - 1 - axis_at))
    return level


def bell_draw(rng, extent, scale, limit, shards=(), kind=jnp.bfloat16):
    level = steps_of(rng, extent, shards, -0.22, 0.18) if shards else 1.0
    values = jax.random.normal(rng, extent, jnp.float32) * scale * level
    return jnp.minimum(jnp.maximum(values, -limit), limit).astype(kind)


def setup_inputs(seed: int = 0) -> dict:
    arg_keys = jax.random.split(jax.random.key(seed), 8)
    residual_in = draw_residual_in(jax.random.fold_in(arg_keys[7], 71), 0)
    gain_in = jnp.clip(1.0 + 0.18 * jax.random.normal(arg_keys[1], (D,), jnp.float32), 0.1, 1.9)
    shift_in = bell_draw(arg_keys[2], (D,), 0.5, 3.0, ((0, 4),), jnp.float32)
    up_weight = bell_draw(arg_keys[3], (D, FF), D ** -0.5, 0.09375, ((0, 4), (1, 2)))
    down_weight = bell_draw(arg_keys[4], (FF, D), FF ** -0.5, 0.046875, ((0, 2), (1, 4)))
    gain_out = jnp.clip(1.0 + 0.18 * jax.random.normal(arg_keys[5], (D,), jnp.float32), 0.1, 1.9)
    shift_out = bell_draw(arg_keys[6], (D,), 0.5, 3.0, ((0, 4),), jnp.float32)
    return {"residual_in": residual_in, "gain_in": gain_in, "shift_in": shift_in, "up_weight": up_weight, "down_weight": down_weight, "gain_out": gain_out, "shift_out": shift_out}


def layer_norm(values, gain, shift):
    mean = lax.optimization_barrier(jnp.mean(values, axis=-1, keepdims=True))
    centred = values - mean
    spread = lax.optimization_barrier(jnp.mean(centred * centred, axis=-1, keepdims=True))
    return centred * jax.lax.rsqrt(spread + 1e-05) * gain + shift

def reference(residual_in, gain_in, shift_in, up_weight, down_weight, gain_out, shift_out):
    normed = layer_norm(residual_in.astype(jnp.float32), gain_in, shift_in).astype(jnp.bfloat16)
    pre = jnp.dot(normed, up_weight, preferred_element_type=jnp.float32)
    hidden = jnp.square(jax.nn.relu(pre)).astype(jnp.bfloat16)
    branch = jnp.dot(hidden, down_weight, preferred_element_type=jnp.float32)
    total = 2.0 ** 0.25 * normed.astype(jnp.float32) + branch
    return layer_norm(total, gain_out, shift_out).astype(jnp.bfloat16)
```

```python
import functools

import jax
import jax.numpy as jnp
from jax import lax
from jax.experimental import pallas as pl
from jax.experimental.pallas import tpu as pltpu
from jax.sharding import PartitionSpec as P

MESH = pl.DeviceIdType.MESH
LANES = 128
STAT_ROWS = 8
EXTRA = 16
ROWS = 64
CHUNK = 512
WINDOW = 4
RAW = 4
LAG = 3
AHEAD = 4
LAG_STEP = 7
TOTAL_AT = 3
NORM_AT = 8
LIMIT = 56


def kernel(
    n, n_ra, x_hbm, gain_in_hbm, shift_in_hbm, gain_out_hbm, shift_out_hbm, up_hbm, down_hbm, out_ref,
    x_v, vectors, up_v, down_v, tile_v, raw, raw_out, raw_in, sums, from_outer, from_partner, normed,
    acc, acc_in, stats_in, stats_out,
    x_sem, vector_sem, up_sem, down_sem, raw_sent, raw_got, sums_sent, outer_got, partner_got,
    hidden_sent, hidden_got, stat_sent, stat_got, acc_sent, acc_got,
):
    me = lax.axis_index("cb")
    ra = lax.axis_index("ra")
    chunks, depth, width = up_v.shape
    tokens = normed.shape[0]
    steps, rows = sums.shape[0], sums.shape[1]
    blocks = tokens // rows
    half = n // 2
    ahead = min(AHEAD, chunks)
    n_raw = raw_out.shape[0]
    side = me // half
    level = me * (1 - side) + (n - 1 - me) * side
    inner = lax.rem(me + 1 - 2 * side + n, n)
    outer = lax.rem(me - 1 + 2 * side + n, n)
    is_mid = level == half - 1
    has_outer = level > 0
    sends_raw = (level == 0) & (half > 1)
    takes_raw = level == 1
    hidden = from_outer

    def block_of(b):
        return pl.ds(pl.multiple_of(b * rows, rows), rows)

    def x_copy(b):
        return pltpu.make_async_copy(x_hbm.at[block_of(b)], x_v.at[block_of(b)], x_sem.at[b])

    def vector_copy(i):
        source = (gain_in_hbm, shift_in_hbm, gain_out_hbm, shift_out_hbm)[i]
        return pltpu.make_async_copy(source, vectors.at[i], vector_sem.at[i])

    def up_copy(c):
        columns = pl.ds(pl.multiple_of(c * width, width), width)
        return pltpu.make_async_copy(up_hbm.at[:, columns], up_v.at[c], up_sem.at[c])

    def down_copy(c):
        units = pl.ds(pl.multiple_of(c * width, width), width)
        return pltpu.make_async_copy(down_hbm.at[units, :], down_v.at[c], down_sem.at[c])

    barrier = pltpu.get_barrier_semaphore()
    for k in range(1, n):
        pl.semaphore_signal(barrier, inc=1, device_id={"cb": lax.rem(me + k, n)}, device_id_type=MESH)
    for k in range(1, n_ra):
        pl.semaphore_signal(barrier, inc=1, device_id={"ra": lax.rem(ra + k, n_ra)}, device_id_type=MESH)

    x_copy(0).start()
    vector_copy(0).start()
    vector_copy(1).start()
    for b in range(1, blocks):
        x_copy(b).start()
    for c in range(ahead):
        up_copy(c).start()
    vector_copy(2).start()
    vector_copy(3).start()

    def row_stats(values):
        total = jnp.sum(values, axis=1, keepdims=True)
        centred = values - total * (1.0 / depth)
        squares = jnp.sum(centred * centred, axis=1, keepdims=True)
        lane = lax.broadcasted_iota(jnp.int32, (values.shape[0], LANES), 1)
        tile_v[pl.ds(0, rows)] = jnp.where(lane == 0, total, jnp.where(lane == 1, squares, 0.0))
        return tile_v[...].T[:STAT_ROWS], centred

    def stat_copy(stats, which, b, k, slot):
        return pltpu.make_async_remote_copy(
            src_ref=stats.at[b, slot], dst_ref=stats.at[b, slot],
            send_sem=stat_sent.at[which, b, k], recv_sem=stat_got.at[which, b, slot],
            device_id={"cb": lax.rem(me + k, n)}, device_id_type=MESH,
        )

    def send_stats(stats, which, b):
        for k in range(1, n):
            stat_copy(stats, which, b, k, me).start()

    def merged_stats(stats, which, b):
        for k in range(1, n):
            stat_copy(stats, which, b, k, lax.rem(me + k, n)).wait_recv()
        for k in range(1, n):
            stat_copy(stats, which, b, k, me).wait_send()
        total = stats[b, 0][0:1]
        for j in range(1, n):
            total = total + stats[b, j][0:1]
        mean = total / (depth * n)
        squares = jnp.zeros_like(mean)
        for j in range(n):
            block = stats[b, j]
            gap = block[0:1] * (1.0 / depth) - mean
            squares = squares + (block[1:2] + depth * (gap * gap))
        scale = lax.rsqrt(squares / (depth * n) + 1e-05)
        shift = stats[b, outer][0:1] * (1.0 / depth) - mean
        row = lax.broadcasted_iota(jnp.int32, (LANES, LANES), 0)
        tile = jnp.where(row == 0, mean, jnp.where(row == 1, scale, jnp.where(row == 2, shift, 0.0)))
        return tile.T[:rows]

    def make_normed(b):
        tile = merged_stats(stats_in, 0, b)
        values = x_v[block_of(b)].astype(jnp.float32)
        normed[block_of(b)] = (
            (values - tile[:, 0:1]) * tile[:, 1:2] * vectors[0] + vectors[1]
        ).astype(jnp.bfloat16)
        return tile

    def raw_copy(c):
        return pltpu.make_async_remote_copy(
            src_ref=raw_out.at[c], dst_ref=raw_in.at[c], send_sem=raw_sent.at[c], recv_sem=raw_got.at[c],
            device_id={"cb": inner}, device_id_type=MESH,
        )

    def sum_copy(s, into, got):
        return pltpu.make_async_remote_copy(
            src_ref=sums.at[s], dst_ref=into.at[s], send_sem=sums_sent.at[s], recv_sem=got.at[s],
            device_id={"cb": inner}, device_id_type=MESH,
        )

    def hidden_copy(s):
        return pltpu.make_async_remote_copy(
            src_ref=hidden.at[s], dst_ref=hidden.at[s], send_sem=hidden_sent.at[s],
            recv_sem=hidden_got.at[s], device_id={"cb": outer}, device_id_type=MESH,
        )

    def acc_copy(k, b):
        return pltpu.make_async_remote_copy(
            src_ref=acc.at[block_of(b)], dst_ref=acc_in.at[k - 1, block_of(b)],
            send_sem=acc_sent.at[k - 1, b], recv_sem=acc_got.at[k - 1, b],
            device_id={"ra": lax.rem(ra + k, n_ra)}, device_id_type=MESH,
        )

    def want_up(c):
        up_copy(c).wait()

        @pl.when(c + ahead < chunks)
        def _():
            up_copy(c + ahead).start()
            down_copy(c + ahead).start()

    tile_v[...] = jnp.zeros_like(tile_v)
    x_copy(0).wait()
    stats_in[0, me], centred = row_stats(x_v[block_of(0)].astype(jnp.float32))
    vector_copy(0).wait()
    vector_copy(1).wait()

    @pl.when(sends_raw)
    def _():
        raw[pl.ds(0, rows)] = (centred * vectors[0]).astype(jnp.bfloat16)
        row = lax.broadcasted_iota(jnp.int32, (EXTRA, depth), 0)
        raw[pl.ds(rows, EXTRA)] = jnp.where(
            row == 0, vectors[0], jnp.where(row == 1, vectors[1], 0.0)
        ).astype(jnp.bfloat16)

    pl.semaphore_wait(barrier, n - 1 + n_ra - 1)
    send_stats(stats_in, 0, 0)

    @pl.when(sends_raw)
    def _():
        @pl.loop(0, n_raw)
        def _(c):
            want_up(c)
            raw_out[c] = jnp.dot(raw[...], up_v[c], preferred_element_type=jnp.float32).astype(jnp.bfloat16)
            raw_copy(c).start()

    @pl.loop(1, blocks)
    def _(b):
        x_copy(b).wait()
        stats_in[b, me] = row_stats(x_v[block_of(b)].astype(jnp.float32))[0]
        send_stats(stats_in, 0, b)

    for c in range(ahead):
        down_copy(c).start()
    acc[...] = jnp.zeros_like(acc)
    tile_v[pl.ds(0, rows)] = make_normed(0)

    @pl.when(~takes_raw)
    def _():
        tile_v[...] = jnp.zeros_like(tile_v)

    def inward(s):
        b, c = s // chunks, lax.rem(s, chunks)

        @pl.when((b == 0) & ((s >= n_raw) | ~sends_raw))
        def _():
            want_up(c)

        def part():
            return jnp.dot(normed[block_of(b)], up_v[c], preferred_element_type=jnp.float32)

        @pl.when(has_outer & ((s >= n_raw) | ~takes_raw))
        def _():
            mine = part()
            sum_copy(s, from_outer, outer_got).wait_recv()
            sums[s] = (mine + from_outer[s].astype(jnp.float32)).astype(jnp.bfloat16)

        @pl.when((s < n_raw) & takes_raw)
        def _():
            mine = part()
            raw_copy(s).wait_recv()
            block = raw_in[s].astype(jnp.float32)
            tile = tile_v[pl.ds(0, rows)]
            theirs = (block[:rows] + tile[:, 2:3] * block[rows : rows + 1]) * tile[:, 1:2]
            sums[s] = (mine + (theirs + block[rows + 1 : rows + 2])).astype(jnp.bfloat16)

        @pl.when((level == 0) & ((s >= n_raw) | ~sends_raw))
        def _():
            sums[s] = part().astype(jnp.bfloat16)

        @pl.when((s >= WINDOW) & ((s >= WINDOW + n_raw) | ~sends_raw))
        def _():
            sum_copy(s - WINDOW, from_outer, outer_got).wait_send()

        @pl.when((s >= WINDOW) & (s < WINDOW + n_raw) & sends_raw)
        def _():
            raw_copy(s - WINDOW).wait_send()

        @pl.when(is_mid)
        def _():
            sum_copy(s, from_partner, partner_got).start()

        @pl.when((level < half - 1) & ((s >= n_raw) | ~sends_raw))
        def _():
            sum_copy(s, from_outer, outer_got).start()

        @pl.when((c == chunks // 2) & (b + 1 < blocks))
        def _():
            make_normed(b + 1)

    def outward(s):
        b, c = s // chunks, lax.rem(s, chunks)

        @pl.when(is_mid)
        def _():
            sum_copy(s, from_partner, partner_got).wait_recv()
            full = sums[s].astype(jnp.float32) + from_partner[s].astype(jnp.float32)
            hidden[s] = jnp.square(jnp.maximum(full, 0.0)).astype(jnp.bfloat16)

        @pl.when(level < half - 1)
        def _():
            hidden_copy(s).wait_recv()

        @pl.when(has_outer)
        def _():
            hidden_copy(s).start()

        @pl.when(b == 0)
        def _():
            down_copy(c).wait()

        acc[block_of(b)] += jnp.dot(hidden[s], down_v[c], preferred_element_type=jnp.float32)

        @pl.when(c == chunks - 1)
        def _():
            for k in range(1, n_ra):
                acc_copy(k, b).start()

        @pl.when((b > 0) & (c == TOTAL_AT))
        def _():
            make_total(b - 1)

        @pl.when((b > 0) & (c == NORM_AT))
        def _():
            make_out(b - 1)

    def make_total(b):
        block = block_of(b)
        for k in range(1, n_ra):
            acc_copy(k, b).wait()
        branch = acc[block]
        for k in range(1, n_ra):
            branch = branch + acc_in[k - 1, block]
        total = 2.0**0.25 * normed[block].astype(jnp.float32) + branch
        acc[block] = total
        stats_out[b, me] = row_stats(total)[0]
        send_stats(stats_out, 1, b)

    def make_out(b):
        tile = merged_stats(stats_out, 1, b)
        out_ref[block_of(b)] = (
            (acc[block_of(b)] - tile[:, 0:1]) * tile[:, 1:2] * vectors[2] + vectors[3]
        ).astype(jnp.bfloat16)

    lag = LAG + LAG_STEP * (half - 1 - level)
    vector_copy(2).wait()
    vector_copy(3).wait()

    @pl.loop(0, steps + lag)
    def _(step):
        @pl.when(step < steps)
        def _():
            inward(step)

        @pl.when(step >= lag)
        def _():
            outward(step - lag)

    make_total(blocks - 1)

    @pl.loop(max(steps - WINDOW, 0), steps)
    def _(s):
        sum_copy(s, from_outer, outer_got).wait_send()

    @pl.when(has_outer)
    def _():
        @pl.loop(0, steps)
        def _(s):
            hidden_copy(s).wait_send()

    make_out(blocks - 1)


def solution(mesh):
    n, n_ra = mesh.shape["cb"], mesh.shape["ra"]

    def per_device(residual_in, gain_in, shift_in, up_weight, down_weight, gain_out, shift_out):
        tokens, depth = residual_in.shape
        units = up_weight.shape[1]
        width = CHUNK if units % CHUNK == 0 else units
        chunks = units // width
        rows = ROWS if tokens % ROWS == 0 else tokens
        blocks = tokens // rows
        n_raw = min(RAW, WINDOW, chunks)
        vmem = pl.BlockSpec(memory_space=pltpu.VMEM)
        hbm = pl.BlockSpec(memory_space=pl.ANY)
        pieces = (chunks * blocks, rows, width)
        vectors = [vector.reshape(1, depth) for vector in (gain_in, shift_in, gain_out, shift_out)]
        operands = [residual_in, *vectors, up_weight, down_weight]
        return pl.pallas_call(
            functools.partial(kernel, n, n_ra),
            out_shape=pltpu.VMEM((tokens, depth), jnp.bfloat16),
            in_specs=[hbm] * 7,
            out_specs=vmem,
            scratch_shapes=[
                pltpu.VMEM((tokens, depth), jnp.bfloat16),
                pltpu.VMEM((4, 1, depth), jnp.float32),
                pltpu.VMEM((chunks, depth, width), jnp.bfloat16),
                pltpu.VMEM((chunks, width, depth), jnp.bfloat16),
                pltpu.VMEM((LANES, LANES), jnp.float32),
                pltpu.VMEM((rows + EXTRA, depth), jnp.bfloat16),
                pltpu.VMEM((n_raw, rows + EXTRA, width), jnp.bfloat16),
                pltpu.VMEM((n_raw, rows + EXTRA, width), jnp.bfloat16),
                pltpu.VMEM(pieces, jnp.bfloat16),
                pltpu.VMEM(pieces, jnp.bfloat16),
                pltpu.VMEM(pieces, jnp.bfloat16),
                pltpu.VMEM((tokens, depth), jnp.bfloat16),
                pltpu.VMEM((tokens, depth), jnp.float32),
                pltpu.VMEM((n_ra - 1, tokens, depth), jnp.float32),
                pltpu.VMEM((blocks, n, STAT_ROWS, LANES), jnp.float32),
                pltpu.VMEM((blocks, n, STAT_ROWS, LANES), jnp.float32),
                pltpu.SemaphoreType.DMA((blocks,)),
                pltpu.SemaphoreType.DMA((4,)),
            ]
            + [pltpu.SemaphoreType.DMA((chunks,))] * 2
            + [pltpu.SemaphoreType.DMA((n_raw,))] * 2
            + [pltpu.SemaphoreType.DMA((chunks * blocks,))] * 5
            + [pltpu.SemaphoreType.DMA((2, blocks, n))] * 2
            + [pltpu.SemaphoreType.DMA((n_ra - 1, blocks))] * 2,
            compiler_params=pltpu.CompilerParams(
                collective_id=0, has_side_effects=True, vmem_limit_bytes=LIMIT * 1024 * 1024
            ),
        )(*(pltpu.with_memory_space_constraint(array, pltpu.HBM) for array in operands))

    in_specs = (P("dp", "cb"), P("cb"), P("cb"), P("cb", "ra"), P("ra", "cb"), P("cb"), P("cb"))
    return jax.shard_map(
        per_device, mesh=mesh, in_specs=in_specs, out_specs=P("dp", "cb"), check_vma=False
    )
```

```python
import functools

import jax
import jax.numpy as jnp
from jax import lax
from jax.experimental import pallas as pl
from jax.experimental.pallas import tpu as pltpu
from jax.sharding import PartitionSpec as P

MESH = pl.DeviceIdType.MESH
LANES = 128
STAT_ROWS = 8
EXTRA = 16
ROWS = 128
CHUNK = 256
RAW = 3
LAG = 2
AHEAD = 8
LAG_STEP = 7
TOTAL_AT = 5
LIMIT = 56


def kernel(
    n, n_ra, x_hbm, gain_in_hbm, shift_in_hbm, gain_out_hbm, shift_out_hbm, up_hbm, down_hbm, out_ref,
    x_v, vectors, up_v, down_v, tile_v, raw, raw_out, raw_in, sums, from_outer, from_partner, normed, mine,
    acc, acc_in, stats_in, stats_out,
    x_sem, vector_sem, up_sem, down_sem, raw_sent, raw_got, sums_sent, outer_got, partner_got,
    hidden_sent, hidden_got, stat_sent, stat_got, acc_sent, acc_got,
):
    me = lax.axis_index("cb")
    ra = lax.axis_index("ra")
    chunks, depth, width = up_v.shape
    tokens = normed.shape[0]
    steps, rows = sums.shape[0], sums.shape[1]
    blocks = tokens // rows
    half = n // 2
    ahead = min(AHEAD, chunks)
    n_raw = raw_out.shape[0]
    side = me // half
    level = me * (1 - side) + (n - 1 - me) * side
    inner = lax.rem(me + 1 - 2 * side + n, n)
    outer = lax.rem(me - 1 + 2 * side + n, n)
    is_mid = level == half - 1
    has_outer = level > 0
    sends_raw = (level == 0) & (half > 1)
    takes_raw = level == 1
    hidden = from_outer

    def block_of(b):
        return pl.ds(pl.multiple_of(b * rows, rows), rows)

    def x_copy(b):
        return pltpu.make_async_copy(x_hbm.at[block_of(b)], x_v.at[block_of(b)], x_sem.at[b])

    def vector_copy(i):
        source = (gain_in_hbm, shift_in_hbm, gain_out_hbm, shift_out_hbm)[i]
        return pltpu.make_async_copy(source, vectors.at[i], vector_sem.at[i])

    def up_copy(c):
        columns = pl.ds(pl.multiple_of(c * width, width), width)
        return pltpu.make_async_copy(up_hbm.at[:, columns], up_v.at[c], up_sem.at[c])

    def down_copy(c):
        units = pl.ds(pl.multiple_of(c * width, width), width)
        return pltpu.make_async_copy(down_hbm.at[units, :], down_v.at[c], down_sem.at[c])

    barrier = pltpu.get_barrier_semaphore()
    for k in range(1, n):
        pl.semaphore_signal(barrier, inc=1, device_id={"cb": lax.rem(me + k, n)}, device_id_type=MESH)
    for k in range(1, n_ra):
        pl.semaphore_signal(barrier, inc=1, device_id={"ra": lax.rem(ra + k, n_ra)}, device_id_type=MESH)

    x_copy(0).start()
    vector_copy(0).start()
    vector_copy(1).start()
    for b in range(1, blocks):
        x_copy(b).start()
    for c in range(ahead):
        up_copy(c).start()
    vector_copy(2).start()
    vector_copy(3).start()

    def row_stats(values):
        total = jnp.sum(values, axis=1, keepdims=True)
        centred = values - total * (1.0 / depth)
        squares = jnp.sum(centred * centred, axis=1, keepdims=True)
        lane = lax.broadcasted_iota(jnp.int32, (values.shape[0], LANES), 1)
        tile_v[pl.ds(0, rows)] = jnp.where(lane == 0, total, jnp.where(lane == 1, squares, 0.0))
        return tile_v[...].T[:STAT_ROWS], centred

    def stat_copy(stats, which, b, k, slot):
        return pltpu.make_async_remote_copy(
            src_ref=stats.at[b, slot], dst_ref=stats.at[b, slot],
            send_sem=stat_sent.at[which, b, k], recv_sem=stat_got.at[which, b, slot],
            device_id={"cb": lax.rem(me + k, n)}, device_id_type=MESH,
        )

    def send_stats(stats, which, b):
        for k in range(1, n):
            stat_copy(stats, which, b, k, me).start()

    def merged_stats(stats, which, b):
        for k in range(1, n):
            stat_copy(stats, which, b, k, lax.rem(me + k, n)).wait_recv()
        for k in range(1, n):
            stat_copy(stats, which, b, k, me).wait_send()
        total = stats[b, 0][0:1]
        for j in range(1, n):
            total = total + stats[b, j][0:1]
        mean = total / (depth * n)
        squares = jnp.zeros_like(mean)
        for j in range(n):
            block = stats[b, j]
            gap = block[0:1] * (1.0 / depth) - mean
            squares = squares + (block[1:2] + depth * (gap * gap))
        scale = lax.rsqrt(squares / (depth * n) + 1e-05)
        shift = stats[b, outer][0:1] * (1.0 / depth) - mean
        row = lax.broadcasted_iota(jnp.int32, (LANES, LANES), 0)
        tile = jnp.where(row == 0, mean, jnp.where(row == 1, scale, jnp.where(row == 2, shift, 0.0)))
        return tile.T[:rows]

    def make_normed(b):
        tile = merged_stats(stats_in, 0, b)
        values = x_v[block_of(b)].astype(jnp.float32)
        normed[block_of(b)] = (
            (values - tile[:, 0:1]) * tile[:, 1:2] * vectors[0] + vectors[1]
        ).astype(jnp.bfloat16)
        return tile

    def raw_copy(c):
        return pltpu.make_async_remote_copy(
            src_ref=raw_out.at[c], dst_ref=raw_in.at[c], send_sem=raw_sent.at[c], recv_sem=raw_got.at[c],
            device_id={"cb": inner}, device_id_type=MESH,
        )

    def sum_copy(s, into, got):
        return pltpu.make_async_remote_copy(
            src_ref=sums.at[s], dst_ref=into.at[s], send_sem=sums_sent.at[s], recv_sem=got.at[s],
            device_id={"cb": inner}, device_id_type=MESH,
        )

    def hidden_copy(s):
        return pltpu.make_async_remote_copy(
            src_ref=hidden.at[s], dst_ref=hidden.at[s], send_sem=hidden_sent.at[s],
            recv_sem=hidden_got.at[s], device_id={"cb": outer}, device_id_type=MESH,
        )

    def acc_copy(k, b):
        return pltpu.make_async_remote_copy(
            src_ref=acc.at[block_of(b)], dst_ref=acc_in.at[k - 1, block_of(b)],
            send_sem=acc_sent.at[k - 1, b], recv_sem=acc_got.at[k - 1, b],
            device_id={"ra": lax.rem(ra + k, n_ra)}, device_id_type=MESH,
        )

    def want_up(c):
        up_copy(c).wait()

        @pl.when(c + ahead < chunks)
        def _():
            up_copy(c + ahead).start()
            down_copy(c + ahead).start()

    def want_down(c):
        down_copy(c).wait()

    tile_v[...] = jnp.zeros_like(tile_v)
    x_copy(0).wait()
    stats_in[0, me], centred = row_stats(x_v[block_of(0)].astype(jnp.float32))
    vector_copy(0).wait()
    vector_copy(1).wait()

    @pl.when(sends_raw)
    def _():
        raw[pl.ds(0, rows)] = (centred * vectors[0]).astype(jnp.bfloat16)
        row = lax.broadcasted_iota(jnp.int32, (EXTRA, depth), 0)
        raw[pl.ds(rows, EXTRA)] = jnp.where(
            row == 0, vectors[0], jnp.where(row == 1, vectors[1], 0.0)
        ).astype(jnp.bfloat16)

    pl.semaphore_wait(barrier, n - 1 + n_ra - 1)
    send_stats(stats_in, 0, 0)

    @pl.when(sends_raw)
    def _():
        @pl.loop(0, n_raw)
        def _(c):
            want_up(c)
            raw_out[c] = jnp.dot(raw[...], up_v[c], preferred_element_type=jnp.float32).astype(jnp.bfloat16)
            raw_copy(c).start()

    @pl.loop(1, blocks)
    def _(b):
        x_copy(b).wait()
        stats_in[b, me] = row_stats(x_v[block_of(b)].astype(jnp.float32))[0]
        send_stats(stats_in, 0, b)

    for c in range(ahead):
        down_copy(c).start()
    acc[...] = jnp.zeros_like(acc)
    tile_v[pl.ds(0, rows)] = make_normed(0)

    @pl.when(~takes_raw)
    def _():
        tile_v[...] = jnp.zeros_like(tile_v)

    def first_pass(s, weight):
        @pl.when(s < chunks)
        def _():
            weight(s)

    def up_part(s):
        b, c = s // chunks, lax.rem(s, chunks)
        return jnp.dot(normed[block_of(b)], up_v[c], preferred_element_type=jnp.float32)

    def add_down(s):
        b, c = s // chunks, lax.rem(s, chunks)
        acc[block_of(b)] += jnp.dot(hidden[s], down_v[c], preferred_element_type=jnp.float32)

    def after_up(s):
        b, c = s // chunks, lax.rem(s, chunks)

        @pl.when((c == chunks // 2) & (b + 1 < blocks))
        def _():
            make_normed(b + 1)

    def after_down(s):
        b, c = s // chunks, lax.rem(s, chunks)

        @pl.when(c == chunks - 1)
        def _():
            for k in range(1, n_ra):
                acc_copy(k, b).start()

        @pl.when((b > 0) & (c == TOTAL_AT))
        def _():
            make_total(b - 1)

    def take_outer(s):
        sum_copy(s, from_outer, outer_got).wait_recv()
        sums[s] = (mine[lax.rem(s, 2)] + from_outer[s].astype(jnp.float32)).astype(jnp.bfloat16)

    def take_raw(s):
        raw_copy(s).wait_recv()
        block = raw_in[s].astype(jnp.float32)
        tile = tile_v[pl.ds(0, rows)]
        theirs = (block[:rows] + tile[:, 2:3] * block[rows : rows + 1]) * tile[:, 1:2]
        sums[s] = (mine[lax.rem(s, 2)] + (theirs + block[rows + 1 : rows + 2])).astype(jnp.bfloat16)

    def give(s, mid):
        if mid:
            sum_copy(s, from_partner, partner_got).start()
        else:
            sum_copy(s, from_outer, outer_got).start()

    def take_hidden(s, mid):
        if mid:
            sum_copy(s, from_partner, partner_got).wait_recv()
            full = sums[s].astype(jnp.float32) + from_partner[s].astype(jnp.float32)
            hidden[s] = jnp.square(jnp.maximum(full, 0.0)).astype(jnp.bfloat16)
        else:
            hidden_copy(s).wait_recv()
        if half > 1:
            hidden_copy(s).start()

    def relay(mid):
        lag = LAG if mid else LAG + LAG_STEP * (half - 1 - level)

        def next_up(s):
            mine[lax.rem(s, 2)] = up_part(s)

        first_pass(0, want_up)
        next_up(0)

        @pl.loop(0, lag + 1)
        def _(s):
            if half > 1:
                @pl.when((s < n_raw) & takes_raw)
                def _():
                    take_raw(s)

                @pl.when((s >= n_raw) | ~takes_raw)
                def _():
                    take_outer(s)
            else:
                sums[s] = mine[lax.rem(s, 2)].astype(jnp.bfloat16)
            give(s, mid)
            first_pass(s + 1, want_up)
            next_up(s + 1)
            after_up(s + 1)

            @pl.when(s == lag)
            def _():
                take_hidden(s - lag, mid)

        @pl.loop(lag + 1, steps - 1)
        def _(s):
            if half > 1:
                take_outer(s)
            else:
                sums[s] = mine[lax.rem(s, 2)].astype(jnp.bfloat16)
            give(s, mid)
            first_pass(s + 1, want_up)
            first_pass(s - lag - 1, want_down)
            add_down(s - lag - 1)
            next_up(s + 1)
            take_hidden(s - lag, mid)
            after_up(s + 1)
            after_down(s - lag - 1)

        if half > 1:
            take_outer(steps - 1)
        else:
            sums[steps - 1] = mine[(steps - 1) % 2].astype(jnp.bfloat16)
        give(steps - 1, mid)

        @pl.loop(steps - 1, steps + lag)
        def _(s):
            first_pass(s - lag - 1, want_down)
            add_down(s - lag - 1)
            after_down(s - lag - 1)
            take_hidden(s - lag, mid)

        first_pass(steps - 1, want_down)
        add_down(steps - 1)
        after_down(steps - 1)

    def source():
        @pl.loop(n_raw, steps)
        def _(s):
            first_pass(s, want_up)
            sums[s] = up_part(s).astype(jnp.bfloat16)
            sum_copy(s, from_outer, outer_got).start()
            after_up(s)

        @pl.loop(0, steps)
        def _(s):
            hidden_copy(s).wait_recv()
            first_pass(s, want_down)
            add_down(s)
            after_down(s)

    def make_total(b):
        block = block_of(b)
        for k in range(1, n_ra):
            acc_copy(k, b).wait()
        branch = acc[block]
        for k in range(1, n_ra):
            branch = branch + acc_in[k - 1, block]
        total = 2.0**0.25 * normed[block].astype(jnp.float32) + branch
        acc[block] = total
        stats_out[b, me] = row_stats(total)[0]
        send_stats(stats_out, 1, b)

    def make_out(b):
        tile = merged_stats(stats_out, 1, b)
        out_ref[block_of(b)] = (
            (acc[block_of(b)] - tile[:, 0:1]) * tile[:, 1:2] * vectors[2] + vectors[3]
        ).astype(jnp.bfloat16)

    vector_copy(2).wait()
    vector_copy(3).wait()
    pl.when(is_mid)(functools.partial(relay, True))
    if half > 1:
        pl.when(level == 0)(source)
    if half > 2:
        pl.when((level > 0) & (level < half - 1))(functools.partial(relay, False))

    make_total(blocks - 1)

    @pl.when(sends_raw)
    def _():
        @pl.loop(0, n_raw)
        def _(c):
            raw_copy(c).wait_send()

    @pl.loop(jnp.where(sends_raw, n_raw, 0), steps)
    def _(s):
        sum_copy(s, from_outer, outer_got).wait_send()

    @pl.when(has_outer)
    def _():
        @pl.loop(0, steps)
        def _(s):
            hidden_copy(s).wait_send()

    @pl.loop(0, blocks)
    def _(b):
        make_out(b)


def solution(mesh):
    n, n_ra = mesh.shape["cb"], mesh.shape["ra"]

    def per_device(residual_in, gain_in, shift_in, up_weight, down_weight, gain_out, shift_out):
        tokens, depth = residual_in.shape
        units = up_weight.shape[1]
        width = CHUNK if units % CHUNK == 0 else units
        chunks = units // width
        rows = ROWS if tokens % ROWS == 0 else tokens
        blocks = tokens // rows
        n_raw = min(RAW, LAG + 1, chunks)
        vmem = pl.BlockSpec(memory_space=pltpu.VMEM)
        hbm = pl.BlockSpec(memory_space=pl.ANY)
        pieces = (chunks * blocks, rows, width)
        vectors = [vector.reshape(1, depth) for vector in (gain_in, shift_in, gain_out, shift_out)]
        operands = [residual_in, *vectors, up_weight, down_weight]
        return pl.pallas_call(
            functools.partial(kernel, n, n_ra),
            out_shape=pltpu.VMEM((tokens, depth), jnp.bfloat16),
            in_specs=[hbm] * 7,
            out_specs=vmem,
            scratch_shapes=[
                pltpu.VMEM((tokens, depth), jnp.bfloat16),
                pltpu.VMEM((4, 1, depth), jnp.float32),
                pltpu.VMEM((chunks, depth, width), jnp.bfloat16),
                pltpu.VMEM((chunks, width, depth), jnp.bfloat16),
                pltpu.VMEM((LANES, LANES), jnp.float32),
                pltpu.VMEM((rows + EXTRA, depth), jnp.bfloat16),
                pltpu.VMEM((n_raw, rows + EXTRA, width), jnp.bfloat16),
                pltpu.VMEM((n_raw, rows + EXTRA, width), jnp.bfloat16),
                pltpu.VMEM(pieces, jnp.bfloat16),
                pltpu.VMEM(pieces, jnp.bfloat16),
                pltpu.VMEM(pieces, jnp.bfloat16),
                pltpu.VMEM((tokens, depth), jnp.bfloat16),
                pltpu.VMEM((2, rows, width), jnp.float32),
                pltpu.VMEM((tokens, depth), jnp.float32),
                pltpu.VMEM((n_ra - 1, tokens, depth), jnp.float32),
                pltpu.VMEM((blocks, n, STAT_ROWS, LANES), jnp.float32),
                pltpu.VMEM((blocks, n, STAT_ROWS, LANES), jnp.float32),
                pltpu.SemaphoreType.DMA((blocks,)),
                pltpu.SemaphoreType.DMA((4,)),
            ]
            + [pltpu.SemaphoreType.DMA((chunks,))] * 2
            + [pltpu.SemaphoreType.DMA((n_raw,))] * 2
            + [pltpu.SemaphoreType.DMA((chunks * blocks,))] * 5
            + [pltpu.SemaphoreType.DMA((2, blocks, n))] * 2
            + [pltpu.SemaphoreType.DMA((n_ra - 1, blocks))] * 2,
            compiler_params=pltpu.CompilerParams(
                collective_id=0, has_side_effects=True, vmem_limit_bytes=LIMIT * 1024 * 1024
            ),
        )(*(pltpu.with_memory_space_constraint(array, pltpu.HBM) for array in operands))

    in_specs = (P("dp", "cb"), P("cb"), P("cb"), P("cb", "ra"), P("ra", "cb"), P("cb"), P("cb"))
    return jax.shard_map(
        per_device, mesh=mesh, in_specs=in_specs, out_specs=P("dp", "cb"), check_vma=False
    )
```

```python
import functools

import jax
import jax.numpy as jnp
from jax import lax
from jax.experimental import pallas as pl
from jax.experimental.pallas import tpu as pltpu
from jax.sharding import PartitionSpec as P

MESH = pl.DeviceIdType.MESH
LANES = 128
STAT_ROWS = 8
EXTRA = 16
ROWS = 128
PARTS = 1
CHUNK = 256
RAW = 3
LAG = 2
AHEAD = 4
LAG_STEP = 7
KEEP = 4
TOTAL_AT = 5
LIMIT = 56


def kernel(
    n, n_ra, parts, x_hbm, gain_in_hbm, shift_in_hbm, gain_out_hbm, shift_out_hbm, up_hbm, down_hbm, out_ref,
    x_v, vectors, up_v, down_v, tile_v, raw, raw_out, raw_in, sums, from_outer, from_partner, normed, mine,
    acc, acc_in, stats_in, stats_out,
    x_sem, vector_sem, up_sem, down_sem, raw_sent, raw_got, sums_sent, outer_got, partner_got,
    hidden_sent, hidden_got, tail_sent, tail_got, stat_sent, stat_got, acc_sent, acc_got,
):
    me = lax.axis_index("cb")
    ra = lax.axis_index("ra")
    chunks, depth, width = up_v.shape
    tokens = normed.shape[0]
    steps, rows = sums.shape[0], sums.shape[1]
    blocks = tokens // rows
    part_rows = rows // parts
    half = n // 2
    ahead = min(AHEAD, chunks)
    n_raw = raw_out.shape[0]
    side = me // half
    level = me * (1 - side) + (n - 1 - me) * side
    inner = lax.rem(me + 1 - 2 * side + n, n)
    outer = lax.rem(me - 1 + 2 * side + n, n)
    is_mid = level == half - 1
    has_outer = level > 0
    sends_raw = (level == 0) & (half > 1)
    takes_raw = level == 1
    hidden = from_outer

    def block_of(b):
        return pl.ds(pl.multiple_of(b * rows, rows), rows)

    def part_of(q):
        return pl.ds(pl.multiple_of(q * part_rows, part_rows), part_rows)

    def x_copy(b):
        return pltpu.make_async_copy(x_hbm.at[block_of(b)], x_v.at[block_of(b)], x_sem.at[b])

    def vector_copy(i):
        source = (gain_in_hbm, shift_in_hbm, gain_out_hbm, shift_out_hbm)[i]
        return pltpu.make_async_copy(source, vectors.at[i], vector_sem.at[i])

    def up_copy(c):
        columns = pl.ds(pl.multiple_of(c * width, width), width)
        return pltpu.make_async_copy(up_hbm.at[:, columns], up_v.at[c], up_sem.at[c])

    def down_copy(c):
        units = pl.ds(pl.multiple_of(c * width, width), width)
        return pltpu.make_async_copy(down_hbm.at[units, :], down_v.at[c], down_sem.at[c])

    barrier = pltpu.get_barrier_semaphore()
    for k in range(1, n):
        pl.semaphore_signal(barrier, inc=1, device_id={"cb": lax.rem(me + k, n)}, device_id_type=MESH)
    for k in range(1, n_ra):
        pl.semaphore_signal(barrier, inc=1, device_id={"ra": lax.rem(ra + k, n_ra)}, device_id_type=MESH)

    x_copy(0).start()
    vector_copy(0).start()
    vector_copy(1).start()
    for b in range(1, blocks):
        x_copy(b).start()
    for c in range(ahead):
        up_copy(c).start()
    vector_copy(2).start()
    vector_copy(3).start()

    def row_stats(values):
        total = jnp.sum(values, axis=1, keepdims=True)
        centred = values - total * (1.0 / depth)
        squares = jnp.sum(centred * centred, axis=1, keepdims=True)
        lane = lax.broadcasted_iota(jnp.int32, (values.shape[0], LANES), 1)
        tile_v[pl.ds(0, values.shape[0])] = jnp.where(lane == 0, total, jnp.where(lane == 1, squares, 0.0))
        return tile_v[...].T[:STAT_ROWS], centred

    def stat_copy(stats, which, b, k, slot, core):
        return pltpu.make_async_remote_copy(
            src_ref=stats.at[b, slot], dst_ref=stats.at[b, slot],
            send_sem=stat_sent.at[which, b, core * n + k], recv_sem=stat_got.at[which, b, slot],
            device_id={"cb": lax.rem(me + k, n), "ra": core}, device_id_type=MESH,
        )

    def for_stats(stats, which, b, act):
        if which == 0:
            for k in range(1, n):
                act(stat_copy(stats, which, b, k, me, ra))
        else:
            @pl.when(ra == n_ra - 1)
            def _():
                for k in range(1, n):
                    for core in range(n_ra):
                        act(stat_copy(stats, which, b, k, me, core))

    def send_stats(stats, which, b):
        for_stats(stats, which, b, lambda copy: copy.start())

    def merged_stats(stats, which, b):
        for k in range(1, n):
            stat_copy(stats, which, b, k, lax.rem(me + k, n), ra).wait_recv()
        for_stats(stats, which, b, lambda copy: copy.wait_send())
        total = stats[b, 0][0:1]
        for j in range(1, n):
            total = total + stats[b, j][0:1]
        mean = total / (depth * n)
        squares = jnp.zeros_like(mean)
        for j in range(n):
            block = stats[b, j]
            gap = block[0:1] * (1.0 / depth) - mean
            squares = squares + (block[1:2] + depth * (gap * gap))
        scale = lax.rsqrt(squares / (depth * n) + 1e-05)
        shift = stats[b, outer][0:1] * (1.0 / depth) - mean
        row = lax.broadcasted_iota(jnp.int32, (LANES, LANES), 0)
        tile = jnp.where(row == 0, mean, jnp.where(row == 1, scale, jnp.where(row == 2, shift, 0.0)))
        return tile.T

    def make_normed(b):
        tile = merged_stats(stats_in, 0, b)[:rows]
        values = x_v[block_of(b)].astype(jnp.float32)
        normed[block_of(b)] = (
            (values - tile[:, 0:1]) * tile[:, 1:2] * vectors[0] + vectors[1]
        ).astype(jnp.bfloat16)
        return tile

    def raw_copy(c):
        return pltpu.make_async_remote_copy(
            src_ref=raw_out.at[c], dst_ref=raw_in.at[c], send_sem=raw_sent.at[c], recv_sem=raw_got.at[c],
            device_id={"cb": inner}, device_id_type=MESH,
        )

    def sum_copy(s, into, got):
        return pltpu.make_async_remote_copy(
            src_ref=sums.at[s], dst_ref=into.at[s], send_sem=sums_sent.at[s], recv_sem=got.at[s],
            device_id={"cb": inner}, device_id_type=MESH,
        )

    def hidden_copy(s):
        return pltpu.make_async_remote_copy(
            src_ref=hidden.at[s], dst_ref=hidden.at[s], send_sem=hidden_sent.at[s],
            recv_sem=hidden_got.at[s], device_id={"cb": outer}, device_id_type=MESH,
        )

    def tail_copy(h):
        piece = hidden.at[steps - 1, pl.ds(h * part_rows, part_rows)]
        return pltpu.make_async_remote_copy(
            src_ref=piece, dst_ref=piece, send_sem=tail_sent.at[h], recv_sem=tail_got.at[h],
            device_id={"cb": outer}, device_id_type=MESH,
        )

    def acc_copy(k, q):
        return pltpu.make_async_remote_copy(
            src_ref=acc.at[part_of(q)], dst_ref=acc_in.at[k - 1, part_of(q)],
            send_sem=acc_sent.at[k - 1, q], recv_sem=acc_got.at[k - 1, q],
            device_id={"ra": lax.rem(ra + k, n_ra)}, device_id_type=MESH,
        )

    def want_up(c):
        up_copy(c).wait()

        @pl.when(c + ahead < chunks)
        def _():
            up_copy(c + ahead).start()
            down_copy(c + ahead).start()

    def want_down(c):
        down_copy(c).wait()

    tile_v[...] = jnp.zeros_like(tile_v)
    x_copy(0).wait()
    stats_in[0, me], centred = row_stats(x_v[block_of(0)].astype(jnp.float32))
    vector_copy(0).wait()
    vector_copy(1).wait()

    @pl.when(sends_raw)
    def _():
        raw[pl.ds(0, rows)] = (centred * vectors[0]).astype(jnp.bfloat16)
        row = lax.broadcasted_iota(jnp.int32, (EXTRA, depth), 0)
        raw[pl.ds(rows, EXTRA)] = jnp.where(
            row == 0, vectors[0], jnp.where(row == 1, vectors[1], 0.0)
        ).astype(jnp.bfloat16)

    pl.semaphore_wait(barrier, n - 1 + n_ra - 1)
    send_stats(stats_in, 0, 0)

    @pl.when(sends_raw)
    def _():
        @pl.loop(0, n_raw)
        def _(c):
            want_up(c)
            raw_out[c] = jnp.dot(raw[...], up_v[c], preferred_element_type=jnp.float32).astype(jnp.bfloat16)
            raw_copy(c).start()

    @pl.loop(1, blocks)
    def _(b):
        x_copy(b).wait()
        stats_in[b, me] = row_stats(x_v[block_of(b)].astype(jnp.float32))[0]
        send_stats(stats_in, 0, b)

    for c in range(ahead):
        down_copy(c).start()
    acc[...] = jnp.zeros_like(acc)
    tile_v[pl.ds(0, rows)] = make_normed(0)

    @pl.when(~takes_raw)
    def _():
        tile_v[...] = jnp.zeros_like(tile_v)

    def first_pass(s, weight):
        if isinstance(s, int) and s >= chunks:
            return

        @pl.when(s < chunks)
        def _():
            weight(s)

    def up_part(s):
        b, c = s // chunks, lax.rem(s, chunks)
        return jnp.dot(normed[block_of(b)], up_v[c], preferred_element_type=jnp.float32)

    def add_down(s):
        b, c = s // chunks, lax.rem(s, chunks)
        acc[block_of(b)] += jnp.dot(hidden[s], down_v[c], preferred_element_type=jnp.float32)

    def after_up(s):
        b, c = s // chunks, lax.rem(s, chunks)

        @pl.when((c == chunks // 2) & (b + 1 < blocks))
        def _():
            make_normed(b + 1)

    def after_down(s):
        b, c = s // chunks, lax.rem(s, chunks)

        @pl.when(c == chunks - 1)
        def _():
            for h in range(parts):
                for k in range(1, n_ra):
                    acc_copy(k, b * parts + h).start()

        @pl.when((b > 0) & (c == min(TOTAL_AT, chunks - 1)))
        def _():
            for h in range(parts):
                make_total((b - 1) * parts + h)

        @pl.when((b > 0) & (c == chunks - 2))
        def _():
            for h in range(parts):
                make_out((b - 1) * parts + h)

    def finish_down(wait):
        first_pass(steps - 1, want_down)
        for h in range(parts):
            if wait:
                tail_copy(h).wait_recv()
            q = (blocks - 1) * parts + h
            acc[part_of(q)] += jnp.dot(
                hidden[steps - 1, pl.ds(h * part_rows, part_rows)], down_v[chunks - 1],
                preferred_element_type=jnp.float32,
            )
            for k in range(1, n_ra):
                acc_copy(k, q).start()

    def take_outer(s):
        sum_copy(s, from_outer, outer_got).wait_recv()
        sums[s] = (mine[lax.rem(s, 2)] + from_outer[s].astype(jnp.float32)).astype(jnp.bfloat16)

    def take_raw(s):
        raw_copy(s).wait_recv()
        block = raw_in[s].astype(jnp.float32)
        tile = tile_v[pl.ds(0, rows)]
        theirs = (block[:rows] + tile[:, 2:3] * block[rows : rows + 1]) * tile[:, 1:2]
        sums[s] = (mine[lax.rem(s, 2)] + (theirs + block[rows + 1 : rows + 2])).astype(jnp.bfloat16)

    def give(s, mid):
        if mid:
            sum_copy(s, from_partner, partner_got).start()
        else:
            sum_copy(s, from_outer, outer_got).start()

    def take_last(mid):
        if mid:
            sum_copy(steps - 1, from_partner, partner_got).wait_recv()
        for h in range(parts):
            piece = pl.ds(h * part_rows, part_rows)
            if mid:
                full = sums[steps - 1, piece].astype(jnp.float32) + from_partner[steps - 1, piece].astype(jnp.float32)
                hidden[steps - 1, piece] = jnp.square(jnp.maximum(full, 0.0)).astype(jnp.bfloat16)
            else:
                tail_copy(h).wait_recv()
            if half > 1:
                tail_copy(h).start()

    def take_hidden(s, mid):
        if mid:
            sum_copy(s, from_partner, partner_got).wait_recv()
            full = sums[s].astype(jnp.float32) + from_partner[s].astype(jnp.float32)
            hidden[s] = jnp.square(jnp.maximum(full, 0.0)).astype(jnp.bfloat16)
        else:
            hidden_copy(s).wait_recv()
        if half > 1:
            hidden_copy(s).start()

    def relay(mid):
        lag = LAG if mid else LAG + LAG_STEP * (half - 1 - level)

        def next_up(s):
            mine[lax.rem(s, 2)] = up_part(s)

        first_pass(0, want_up)
        next_up(0)

        @pl.loop(0, lag + 1)
        def _(s):
            if half > 1:
                @pl.when((s < n_raw) & takes_raw)
                def _():
                    take_raw(s)

                @pl.when((s >= n_raw) | ~takes_raw)
                def _():
                    take_outer(s)
            else:
                sums[s] = mine[lax.rem(s, 2)].astype(jnp.bfloat16)
            give(s, mid)
            first_pass(s + 1, want_up)
            next_up(s + 1)
            after_up(s + 1)

            @pl.when(s == lag)
            def _():
                take_hidden(s - lag, mid)

        @pl.loop(lag + 1, steps - 1)
        def _(s):
            if half > 1:
                take_outer(s)
            else:
                sums[s] = mine[lax.rem(s, 2)].astype(jnp.bfloat16)
            give(s, mid)
            first_pass(s + 1, want_up)
            first_pass(s - lag - 1, want_down)
            add_down(s - lag - 1)
            next_up(s + 1)
            take_hidden(s - lag, mid)
            sum_copy(s - lag - 1, from_outer, outer_got).wait_send()
            if half > 1:
                @pl.when(s > lag + KEEP)
                def _():
                    hidden_copy(s - lag - 1 - KEEP).wait_send()
            after_up(s + 1)
            after_down(s - lag - 1)

        if half > 1:
            take_outer(steps - 1)
        else:
            sums[steps - 1] = mine[(steps - 1) % 2].astype(jnp.bfloat16)
        give(steps - 1, mid)

        @pl.loop(steps - 1, steps + lag - 1)
        def _(s):
            first_pass(s - lag - 1, want_down)
            add_down(s - lag - 1)
            after_down(s - lag - 1)
            take_hidden(s - lag, mid)

        first_pass(steps - 2, want_down)
        add_down(steps - 2)
        after_down(steps - 2)
        take_last(mid)
        finish_down(False)

    def source():
        @pl.loop(n_raw, steps)
        def _(s):
            first_pass(s, want_up)
            sums[s] = up_part(s).astype(jnp.bfloat16)
            sum_copy(s, from_outer, outer_got).start()
            after_up(s)

        @pl.loop(0, steps - 1)
        def _(s):
            hidden_copy(s).wait_recv()
            first_pass(s, want_down)
            add_down(s)

            @pl.when(s < n_raw)
            def _():
                raw_copy(s).wait_send()

            @pl.when(s >= n_raw)
            def _():
                sum_copy(s, from_outer, outer_got).wait_send()
            after_down(s)

        finish_down(True)

    def make_total(q):
        block = part_of(q)
        for k in range(1, n_ra):
            acc_copy(k, q).wait()
        branch = acc[block]
        for k in range(1, n_ra):
            branch = branch + acc_in[k - 1, block]
        total = 2.0**0.25 * normed[block].astype(jnp.float32) + branch
        acc[block] = total
        stats_out[q, me] = row_stats(total)[0]
        send_stats(stats_out, 1, q)

    def make_out(q):
        tile = merged_stats(stats_out, 1, q)[:part_rows]
        out_ref[part_of(q)] = (
            (acc[part_of(q)] - tile[:, 0:1]) * tile[:, 1:2] * vectors[2] + vectors[3]
        ).astype(jnp.bfloat16)

    vector_copy(2).wait()
    vector_copy(3).wait()
    pl.when(is_mid)(functools.partial(relay, True))
    if half > 1:
        pl.when(level == 0)(source)
    if half > 2:
        pl.when((level > 0) & (level < half - 1))(functools.partial(relay, False))

    for h in range(parts):
        make_total((blocks - 1) * parts + h)

    lag = LAG + jnp.where(is_mid, 0, LAG_STEP * (half - 1 - level))

    @pl.loop(jnp.where(sends_raw, steps - 1, steps - lag - 2), steps)
    def _(s):
        sum_copy(s, from_outer, outer_got).wait_send()

    @pl.when(has_outer)
    def _():
        @pl.loop(steps - lag - 2 - KEEP, steps - 1)
        def _(s):
            hidden_copy(s).wait_send()

        for h in range(parts):
            tail_copy(h).wait_send()

    for h in range(parts):
        make_out((blocks - 1) * parts + h)


def solution(mesh):
    n, n_ra = mesh.shape["cb"], mesh.shape["ra"]

    def per_device(residual_in, gain_in, shift_in, up_weight, down_weight, gain_out, shift_out):
        tokens, depth = residual_in.shape
        units = up_weight.shape[1]
        width = CHUNK if units % CHUNK == 0 else units
        chunks = units // width
        rows = ROWS if tokens % ROWS == 0 else tokens
        blocks = tokens // rows
        parts = PARTS if rows % (PARTS * 16) == 0 else 1
        n_raw = min(RAW, LAG + 1, chunks)
        vmem = pl.BlockSpec(memory_space=pltpu.VMEM)
        hbm = pl.BlockSpec(memory_space=pl.ANY)
        pieces = (chunks * blocks, rows, width)
        vectors = [vector.reshape(1, depth) for vector in (gain_in, shift_in, gain_out, shift_out)]
        operands = [residual_in, *vectors, up_weight, down_weight]
        return pl.pallas_call(
            functools.partial(kernel, n, n_ra, parts),
            out_shape=pltpu.VMEM((tokens, depth), jnp.bfloat16),
            in_specs=[hbm] * 7,
            out_specs=vmem,
            scratch_shapes=[
                pltpu.VMEM((tokens, depth), jnp.bfloat16),
                pltpu.VMEM((4, 1, depth), jnp.float32),
                pltpu.VMEM((chunks, depth, width), jnp.bfloat16),
                pltpu.VMEM((chunks, width, depth), jnp.bfloat16),
                pltpu.VMEM((LANES, LANES), jnp.float32),
                pltpu.VMEM((rows + EXTRA, depth), jnp.bfloat16),
                pltpu.VMEM((n_raw, rows + EXTRA, width), jnp.bfloat16),
                pltpu.VMEM((n_raw, rows + EXTRA, width), jnp.bfloat16),
                pltpu.VMEM(pieces, jnp.bfloat16),
                pltpu.VMEM(pieces, jnp.bfloat16),
                pltpu.VMEM(pieces, jnp.bfloat16),
                pltpu.VMEM((tokens, depth), jnp.bfloat16),
                pltpu.VMEM((2, rows, width), jnp.float32),
                pltpu.VMEM((tokens, depth), jnp.float32),
                pltpu.VMEM((n_ra - 1, tokens, depth), jnp.float32),
                pltpu.VMEM((blocks, n, STAT_ROWS, LANES), jnp.float32),
                pltpu.VMEM((blocks * parts, n, STAT_ROWS, LANES), jnp.float32),
                pltpu.SemaphoreType.DMA((blocks,)),
                pltpu.SemaphoreType.DMA((4,)),
            ]
            + [pltpu.SemaphoreType.DMA((chunks,))] * 2
            + [pltpu.SemaphoreType.DMA((n_raw,))] * 2
            + [pltpu.SemaphoreType.DMA((chunks * blocks,))] * 5
            + [pltpu.SemaphoreType.DMA((parts,))] * 2
            + [pltpu.SemaphoreType.DMA((2, blocks * parts, n_ra * n)), pltpu.SemaphoreType.DMA((2, blocks * parts, n))]
            + [pltpu.SemaphoreType.DMA((n_ra - 1, blocks * parts))] * 2,
            compiler_params=pltpu.CompilerParams(
                collective_id=0, has_side_effects=True, vmem_limit_bytes=LIMIT * 1024 * 1024
            ),
        )(*(pltpu.with_memory_space_constraint(array, pltpu.HBM) for array in operands))

    in_specs = (P("dp", "cb"), P("cb"), P("cb"), P("cb", "ra"), P("ra", "cb"), P("cb"), P("cb"))
    return jax.shard_map(
        per_device, mesh=mesh, in_specs=in_specs, out_specs=P("dp", "cb"), check_vma=False
    )
```

```python
import functools

import jax
import jax.numpy as jnp
from jax import lax
from jax.experimental import pallas as pl
from jax.experimental.pallas import tpu as pltpu
from jax.sharding import PartitionSpec as P

MESH = pl.DeviceIdType.MESH
LANES = 128
STAT_ROWS = 8
EXTRA = 16
ROWS = 128
PARTS = 1
CHUNK = 256
RAW = 3
LAG = 2
AHEAD = 4
LAG_STEP = 7
KEEP = 4
TOTAL_AT = 5
LIMIT = 56


def kernel(
    n, n_ra, parts, x_hbm, gain_in_hbm, shift_in_hbm, gain_out_hbm, shift_out_hbm, up_hbm, down_hbm, out_ref,
    x_v, vectors, up_v, down_v, tile_v, raw, raw_out, raw_in, sums, from_outer, from_partner, normed, mine,
    acc, acc_in, stats_in, stats_out,
    x_sem, vector_sem, up_sem, down_sem, raw_sent, raw_got, sums_sent, outer_got, partner_got,
    hidden_sent, hidden_got, tail_sent, tail_got, stat_sent, stat_got, acc_sent, acc_got,
):
    me = lax.axis_index("cb")
    ra = lax.axis_index("ra")
    chunks, depth, width = up_v.shape
    tokens = normed.shape[0]
    steps, rows = sums.shape[0], sums.shape[1]
    blocks = tokens // rows
    part_rows = rows // parts
    half = n // 2
    ahead = min(AHEAD, chunks)
    n_raw = raw_out.shape[0]
    side = me // half
    level = me * (1 - side) + (n - 1 - me) * side
    inner = lax.rem(me + 1 - 2 * side + n, n)
    outer = lax.rem(me - 1 + 2 * side + n, n)
    is_mid = level == half - 1
    has_outer = level > 0
    sends_raw = (level == 0) & (half > 1)
    takes_raw = level == 1
    hidden = from_outer

    def block_of(b):
        return pl.ds(pl.multiple_of(b * rows, rows), rows)

    def part_of(q):
        return pl.ds(pl.multiple_of(q * part_rows, part_rows), part_rows)

    def x_copy(b):
        return pltpu.make_async_copy(x_hbm.at[block_of(b)], x_v.at[block_of(b)], x_sem.at[b])

    def vector_copy(i):
        source = (gain_in_hbm, shift_in_hbm, gain_out_hbm, shift_out_hbm)[i]
        return pltpu.make_async_copy(source, vectors.at[i], vector_sem.at[i])

    def up_copy(c):
        columns = pl.ds(pl.multiple_of(c * width, width), width)
        return pltpu.make_async_copy(up_hbm.at[:, columns], up_v.at[c], up_sem.at[c])

    def down_copy(c):
        units = pl.ds(pl.multiple_of(c * width, width), width)
        return pltpu.make_async_copy(down_hbm.at[units, :], down_v.at[c], down_sem.at[c])

    barrier = pltpu.get_barrier_semaphore()
    for k in range(1, n):
        pl.semaphore_signal(barrier, inc=1, device_id={"cb": lax.rem(me + k, n)}, device_id_type=MESH)
    for k in range(1, n_ra):
        pl.semaphore_signal(barrier, inc=1, device_id={"ra": lax.rem(ra + k, n_ra)}, device_id_type=MESH)

    x_copy(0).start()
    vector_copy(0).start()
    vector_copy(1).start()
    for b in range(1, blocks):
        x_copy(b).start()
    for c in range(ahead):
        up_copy(c).start()
    vector_copy(2).start()
    vector_copy(3).start()

    def row_stats(values):
        total = jnp.sum(values, axis=1, keepdims=True)
        centred = values - total * (1.0 / depth)
        squares = jnp.sum(centred * centred, axis=1, keepdims=True)
        lane = lax.broadcasted_iota(jnp.int32, (values.shape[0], LANES), 1)
        tile_v[pl.ds(0, values.shape[0])] = jnp.where(lane == 0, total, jnp.where(lane == 1, squares, 0.0))
        return tile_v[...].T[:STAT_ROWS], centred

    def stat_copy(stats, which, b, k, slot, core):
        return pltpu.make_async_remote_copy(
            src_ref=stats.at[b, slot], dst_ref=stats.at[b, slot],
            send_sem=stat_sent.at[which, b, core * n + k], recv_sem=stat_got.at[which, b, slot],
            device_id={"cb": lax.rem(me + k, n), "ra": core}, device_id_type=MESH,
        )

    def for_stats(stats, which, b, act):
        if which == 0:
            for k in range(1, n):
                act(stat_copy(stats, which, b, k, me, ra))
        else:
            @pl.when(ra == n_ra - 1)
            def _():
                for k in range(1, n):
                    for core in range(n_ra):
                        act(stat_copy(stats, which, b, k, me, core))

    def send_stats(stats, which, b):
        for_stats(stats, which, b, lambda copy: copy.start())

    def merged_stats(stats, which, b):
        for k in range(1, n):
            stat_copy(stats, which, b, k, lax.rem(me + k, n), ra).wait_recv()
        for_stats(stats, which, b, lambda copy: copy.wait_send())
        total = stats[b, 0][0:1]
        for j in range(1, n):
            total = total + stats[b, j][0:1]
        mean = total / (depth * n)
        squares = jnp.zeros_like(mean)
        for j in range(n):
            block = stats[b, j]
            gap = block[0:1] * (1.0 / depth) - mean
            squares = squares + (block[1:2] + depth * (gap * gap))
        scale = lax.rsqrt(squares / (depth * n) + 1e-05)
        shift = stats[b, outer][0:1] * (1.0 / depth) - mean
        row = lax.broadcasted_iota(jnp.int32, (LANES, LANES), 0)
        tile = jnp.where(row == 0, mean, jnp.where(row == 1, scale, jnp.where(row == 2, shift, 0.0)))
        return tile.T

    def make_normed(b):
        tile = merged_stats(stats_in, 0, b)[:rows]
        values = x_v[block_of(b)].astype(jnp.float32)
        normed[block_of(b)] = (
            (values - tile[:, 0:1]) * tile[:, 1:2] * vectors[0] + vectors[1]
        ).astype(jnp.bfloat16)
        return tile

    def raw_copy(c):
        return pltpu.make_async_remote_copy(
            src_ref=raw_out.at[c], dst_ref=raw_in.at[c], send_sem=raw_sent.at[c], recv_sem=raw_got.at[c],
            device_id={"cb": inner}, device_id_type=MESH,
        )

    def sum_copy(s, into, got):
        return pltpu.make_async_remote_copy(
            src_ref=sums.at[s], dst_ref=into.at[s], send_sem=sums_sent.at[s], recv_sem=got.at[s],
            device_id={"cb": inner}, device_id_type=MESH,
        )

    def hidden_copy(s):
        return pltpu.make_async_remote_copy(
            src_ref=hidden.at[s], dst_ref=hidden.at[s], send_sem=hidden_sent.at[s],
            recv_sem=hidden_got.at[s], device_id={"cb": outer}, device_id_type=MESH,
        )

    def tail_copy(h):
        piece = hidden.at[steps - 1, pl.ds(h * part_rows, part_rows)]
        return pltpu.make_async_remote_copy(
            src_ref=piece, dst_ref=piece, send_sem=tail_sent.at[h], recv_sem=tail_got.at[h],
            device_id={"cb": outer}, device_id_type=MESH,
        )

    def acc_copy(k, q):
        return pltpu.make_async_remote_copy(
            src_ref=acc.at[part_of(q)], dst_ref=acc_in.at[k - 1, part_of(q)],
            send_sem=acc_sent.at[k - 1, q], recv_sem=acc_got.at[k - 1, q],
            device_id={"ra": lax.rem(ra + k, n_ra)}, device_id_type=MESH,
        )

    def want_up(c):
        up_copy(c).wait()

        @pl.when(c + ahead < chunks)
        def _():
            up_copy(c + ahead).start()
            down_copy(c + ahead).start()

    def want_down(c):
        down_copy(c).wait()

    tile_v[...] = jnp.zeros_like(tile_v)
    x_copy(0).wait()
    stats_in[0, me], centred = row_stats(x_v[block_of(0)].astype(jnp.float32))
    vector_copy(0).wait()
    vector_copy(1).wait()

    @pl.when(sends_raw)
    def _():
        raw[pl.ds(0, rows)] = (centred * vectors[0]).astype(jnp.bfloat16)
        row = lax.broadcasted_iota(jnp.int32, (EXTRA, depth), 0)
        raw[pl.ds(rows, EXTRA)] = jnp.where(
            row == 0, vectors[0], jnp.where(row == 1, vectors[1], 0.0)
        ).astype(jnp.bfloat16)

    def raw_part(c):
        want_up(c)
        raw_out[c] = jnp.dot(raw[...], up_v[c], preferred_element_type=jnp.float32).astype(jnp.bfloat16)

    @pl.when(sends_raw)
    def _():
        raw_part(0)

    pl.semaphore_wait(barrier, n - 1 + n_ra - 1)
    send_stats(stats_in, 0, 0)

    @pl.when(sends_raw)
    def _():
        raw_copy(0).start()

        @pl.loop(1, n_raw)
        def _(c):
            raw_part(c)
            raw_copy(c).start()

    @pl.loop(1, blocks)
    def _(b):
        x_copy(b).wait()
        stats_in[b, me] = row_stats(x_v[block_of(b)].astype(jnp.float32))[0]
        send_stats(stats_in, 0, b)

    for c in range(ahead):
        down_copy(c).start()
    acc[...] = jnp.zeros_like(acc)
    tile_v[pl.ds(0, rows)] = make_normed(0)

    @pl.when(~takes_raw)
    def _():
        tile_v[...] = jnp.zeros_like(tile_v)

    def first_pass(s, weight):
        if isinstance(s, int) and s >= chunks:
            return

        @pl.when(s < chunks)
        def _():
            weight(s)

    def up_part(s):
        b, c = s // chunks, lax.rem(s, chunks)
        return jnp.dot(normed[block_of(b)], up_v[c], preferred_element_type=jnp.float32)

    def add_down(s):
        b, c = s // chunks, lax.rem(s, chunks)
        acc[block_of(b)] += jnp.dot(hidden[s], down_v[c], preferred_element_type=jnp.float32)

    def after_up(s):
        b, c = s // chunks, lax.rem(s, chunks)

        @pl.when((c == chunks // 2) & (b + 1 < blocks))
        def _():
            make_normed(b + 1)

    def after_down(s):
        b, c = s // chunks, lax.rem(s, chunks)

        @pl.when(c == chunks - 1)
        def _():
            for h in range(parts):
                for k in range(1, n_ra):
                    acc_copy(k, b * parts + h).start()

        @pl.when((b > 0) & (c == min(TOTAL_AT, chunks - 1)))
        def _():
            for h in range(parts):
                make_total((b - 1) * parts + h)

        @pl.when((b > 0) & (c == chunks - 2))
        def _():
            for h in range(parts):
                make_out((b - 1) * parts + h)

    def finish_down(wait):
        first_pass(steps - 1, want_down)
        for h in range(parts):
            if wait:
                tail_copy(h).wait_recv()
            q = (blocks - 1) * parts + h
            acc[part_of(q)] += jnp.dot(
                hidden[steps - 1, pl.ds(h * part_rows, part_rows)], down_v[chunks - 1],
                preferred_element_type=jnp.float32,
            )
            for k in range(1, n_ra):
                acc_copy(k, q).start()

    def take_outer(s):
        sum_copy(s, from_outer, outer_got).wait_recv()
        sums[s] = (mine[lax.rem(s, 2)] + from_outer[s].astype(jnp.float32)).astype(jnp.bfloat16)

    def take_raw(s):
        raw_copy(s).wait_recv()
        block = raw_in[s].astype(jnp.float32)
        tile = tile_v[pl.ds(0, rows)]
        theirs = (block[:rows] + tile[:, 2:3] * block[rows : rows + 1]) * tile[:, 1:2]
        sums[s] = (mine[lax.rem(s, 2)] + (theirs + block[rows + 1 : rows + 2])).astype(jnp.bfloat16)

    def give(s, mid):
        if mid:
            sum_copy(s, from_partner, partner_got).start()
        else:
            sum_copy(s, from_outer, outer_got).start()

    def take_last(mid):
        if mid:
            sum_copy(steps - 1, from_partner, partner_got).wait_recv()
        for h in range(parts):
            piece = pl.ds(h * part_rows, part_rows)
            if mid:
                full = sums[steps - 1, piece].astype(jnp.float32) + from_partner[steps - 1, piece].astype(jnp.float32)
                hidden[steps - 1, piece] = jnp.square(jnp.maximum(full, 0.0)).astype(jnp.bfloat16)
            else:
                tail_copy(h).wait_recv()
            if half > 1:
                tail_copy(h).start()

    def take_hidden(s, mid):
        if mid:
            sum_copy(s, from_partner, partner_got).wait_recv()
            full = sums[s].astype(jnp.float32) + from_partner[s].astype(jnp.float32)
            hidden[s] = jnp.square(jnp.maximum(full, 0.0)).astype(jnp.bfloat16)
        else:
            hidden_copy(s).wait_recv()
        if half > 1:
            hidden_copy(s).start()

    def relay(mid):
        lag = LAG if mid else LAG + LAG_STEP * (half - 1 - level)

        def next_up(s):
            mine[lax.rem(s, 2)] = up_part(s)

        first_pass(0, want_up)
        next_up(0)

        @pl.loop(0, lag + 1)
        def _(s):
            if half > 1:
                @pl.when((s < n_raw) & takes_raw)
                def _():
                    take_raw(s)

                @pl.when((s >= n_raw) | ~takes_raw)
                def _():
                    take_outer(s)
            else:
                sums[s] = mine[lax.rem(s, 2)].astype(jnp.bfloat16)
            give(s, mid)
            first_pass(s + 1, want_up)
            next_up(s + 1)
            after_up(s + 1)

            @pl.when(s == lag)
            def _():
                take_hidden(s - lag, mid)

        @pl.loop(lag + 1, steps - 1)
        def _(s):
            if half > 1:
                take_outer(s)
            else:
                sums[s] = mine[lax.rem(s, 2)].astype(jnp.bfloat16)
            give(s, mid)
            first_pass(s + 1, want_up)
            first_pass(s - lag - 1, want_down)
            add_down(s - lag - 1)
            next_up(s + 1)
            take_hidden(s - lag, mid)
            sum_copy(s - lag - 1, from_outer, outer_got).wait_send()
            if half > 1:
                @pl.when(s > lag + KEEP)
                def _():
                    hidden_copy(s - lag - 1 - KEEP).wait_send()
            after_up(s + 1)
            after_down(s - lag - 1)

        if half > 1:
            take_outer(steps - 1)
        else:
            sums[steps - 1] = mine[(steps - 1) % 2].astype(jnp.bfloat16)
        give(steps - 1, mid)

        @pl.loop(steps - 1, steps + lag - 1)
        def _(s):
            first_pass(s - lag - 1, want_down)
            add_down(s - lag - 1)
            after_down(s - lag - 1)
            take_hidden(s - lag, mid)

        first_pass(steps - 2, want_down)
        add_down(steps - 2)
        after_down(steps - 2)
        take_last(mid)
        finish_down(False)

    def source():
        @pl.loop(n_raw, steps)
        def _(s):
            first_pass(s, want_up)
            sums[s] = up_part(s).astype(jnp.bfloat16)
            sum_copy(s, from_outer, outer_got).start()
            after_up(s)

        @pl.loop(0, steps - 1)
        def _(s):
            hidden_copy(s).wait_recv()
            first_pass(s, want_down)
            add_down(s)

            @pl.when(s < n_raw)
            def _():
                raw_copy(s).wait_send()

            @pl.when(s >= n_raw)
            def _():
                sum_copy(s, from_outer, outer_got).wait_send()
            after_down(s)

        finish_down(True)

    def make_total(q):
        block = part_of(q)
        for k in range(1, n_ra):
            acc_copy(k, q).wait()
        branch = acc[block]
        for k in range(1, n_ra):
            branch = branch + acc_in[k - 1, block]
        total = 2.0**0.25 * normed[block].astype(jnp.float32) + branch
        acc[block] = total
        stats_out[q, me] = row_stats(total)[0]
        send_stats(stats_out, 1, q)

    def make_out(q):
        tile = merged_stats(stats_out, 1, q)[:part_rows]
        out_ref[part_of(q)] = (
            (acc[part_of(q)] - tile[:, 0:1]) * tile[:, 1:2] * vectors[2] + vectors[3]
        ).astype(jnp.bfloat16)

    vector_copy(2).wait()
    vector_copy(3).wait()
    pl.when(is_mid)(functools.partial(relay, True))
    if half > 1:
        pl.when(level == 0)(source)
    if half > 2:
        pl.when((level > 0) & (level < half - 1))(functools.partial(relay, False))

    for h in range(parts):
        make_total((blocks - 1) * parts + h)

    lag = LAG + jnp.where(is_mid, 0, LAG_STEP * (half - 1 - level))

    @pl.loop(jnp.where(sends_raw, steps - 1, steps - lag - 2), steps)
    def _(s):
        sum_copy(s, from_outer, outer_got).wait_send()

    @pl.when(has_outer)
    def _():
        @pl.loop(steps - lag - 2 - KEEP, steps - 1)
        def _(s):
            hidden_copy(s).wait_send()

        for h in range(parts):
            tail_copy(h).wait_send()

    for h in range(parts):
        make_out((blocks - 1) * parts + h)


def solution(mesh):
    n, n_ra = mesh.shape["cb"], mesh.shape["ra"]

    def per_device(residual_in, gain_in, shift_in, up_weight, down_weight, gain_out, shift_out):
        tokens, depth = residual_in.shape
        units = up_weight.shape[1]
        width = CHUNK if units % CHUNK == 0 else units
        chunks = units // width
        rows = ROWS if tokens % ROWS == 0 else tokens
        blocks = tokens // rows
        parts = PARTS if rows % (PARTS * 16) == 0 else 1
        n_raw = min(RAW, LAG + 1, chunks)
        vmem = pl.BlockSpec(memory_space=pltpu.VMEM)
        hbm = pl.BlockSpec(memory_space=pl.ANY)
        pieces = (chunks * blocks, rows, width)
        vectors = [vector.reshape(1, depth) for vector in (gain_in, shift_in, gain_out, shift_out)]
        operands = [residual_in, *vectors, up_weight, down_weight]
        return pl.pallas_call(
            functools.partial(kernel, n, n_ra, parts),
            out_shape=pltpu.VMEM((tokens, depth), jnp.bfloat16),
            in_specs=[hbm] * 7,
            out_specs=vmem,
            scratch_shapes=[
                pltpu.VMEM((tokens, depth), jnp.bfloat16),
                pltpu.VMEM((4, 1, depth), jnp.float32),
                pltpu.VMEM((chunks, depth, width), jnp.bfloat16),
                pltpu.VMEM((chunks, width, depth), jnp.bfloat16),
                pltpu.VMEM((LANES, LANES), jnp.float32),
                pltpu.VMEM((rows + EXTRA, depth), jnp.bfloat16),
                pltpu.VMEM((n_raw, rows + EXTRA, width), jnp.bfloat16),
                pltpu.VMEM((n_raw, rows + EXTRA, width), jnp.bfloat16),
                pltpu.VMEM(pieces, jnp.bfloat16),
                pltpu.VMEM(pieces, jnp.bfloat16),
                pltpu.VMEM(pieces, jnp.bfloat16),
                pltpu.VMEM((tokens, depth), jnp.bfloat16),
                pltpu.VMEM((2, rows, width), jnp.float32),
                pltpu.VMEM((tokens, depth), jnp.float32),
                pltpu.VMEM((n_ra - 1, tokens, depth), jnp.float32),
                pltpu.VMEM((blocks, n, STAT_ROWS, LANES), jnp.float32),
                pltpu.VMEM((blocks * parts, n, STAT_ROWS, LANES), jnp.float32),
                pltpu.SemaphoreType.DMA((blocks,)),
                pltpu.SemaphoreType.DMA((4,)),
            ]
            + [pltpu.SemaphoreType.DMA((chunks,))] * 2
            + [pltpu.SemaphoreType.DMA((n_raw,))] * 2
            + [pltpu.SemaphoreType.DMA((chunks * blocks,))] * 5
            + [pltpu.SemaphoreType.DMA((parts,))] * 2
            + [pltpu.SemaphoreType.DMA((2, blocks * parts, n_ra * n)), pltpu.SemaphoreType.DMA((2, blocks * parts, n))]
            + [pltpu.SemaphoreType.DMA((n_ra - 1, blocks * parts))] * 2,
            compiler_params=pltpu.CompilerParams(
                collective_id=0, has_side_effects=True, vmem_limit_bytes=LIMIT * 1024 * 1024
            ),
        )(*(pltpu.with_memory_space_constraint(array, pltpu.HBM) for array in operands))

    in_specs = (P("dp", "cb"), P("cb"), P("cb"), P("cb", "ra"), P("ra", "cb"), P("cb"), P("cb"))
    return jax.shard_map(
        per_device, mesh=mesh, in_specs=in_specs, out_specs=P("dp", "cb"), check_vma=False
    )
```
